32 devices in a mesh: sp: 16 (over z, y, x), tp: 2 (over core).
Axes of the slice: x: 2, y: 2, z: 4, core: 2. Of those that a mesh axis runs over, the one named last changes fastest.
Arguments:
- out_grad: bfloat16 [3584, 2048], P('sp'), may hold values from -6 to 6
- moe_input: bfloat16 [3584, 2048], P('sp'), may hold values from -6 to 6
- routes: int32 [3584, 2], P('sp'), may hold values from 0 to 15, all different within a row; in each aligned block of 224 rows (0 to 223, 224 to 447, ...) at most 56 rows name the same one
- route_weights: float32 [3584, 2], P('sp'), may hold values from 0.2 to 1
- conv_result: bfloat16 [3584, 1024], P('sp', 'tp'), may hold values from -60 to 60
- glu_value: bfloat16 [3584, 1024], P('sp', 'tp'), may hold values from -6 to 6
- glu_gate: bfloat16 [3584, 1024], P('sp', 'tp'), may hold values from -6 to 6
- conv_taps: bfloat16 [31, 1024], P(None, 'tp'), may hold values from -1 to 1
- norm_gain: float32 [1024], P('tp'), may hold values from 0.1 to 1.9
- proj_weight: bfloat16 [2048, 1024], P(None, 'tp'), may hold values from -0.1875 to 0.1875
- expert_gate: bfloat16 [16, 2048, 1024], P('sp', None, 'tp'), may hold values from -0.125 to 0.125
- expert_up: bfloat16 [16, 2048, 1024], P('sp', None, 'tp'), may hold values from -0.125 to 0.125
- expert_down: bfloat16 [16, 1024, 2048], P('sp', 'tp'), may hold values from -0.1875 to 0.1875
Outputs:
- input_grad: bfloat16 [3584, 2048], P('sp')
- proj_grad: float32 [2048, 1024], P('sp', 'tp')
- gate_grad: float32 [16, 2048, 1024], P('sp', None, 'tp')
- up_grad: float32 [16, 2048, 1024], P('sp', None, 'tp')
- down_grad: float32 [16, 1024, 2048], P('sp', 'tp')
- value_grad: bfloat16 [3584, 1024], P('sp', 'tp')
- gate_side_grad: bfloat16 [3584, 1024], P('sp', 'tp')
The draws below stay inside these ranges and needn't reach their ends.
Inputs may be any that keep to these rules, and one draw needn't show every extreme that they name: `routes`: in each aligned block of 224 tokens no expert is named more than 56 times, a bound that some block reaches; a token's experts differ.
All inputs are finite; a program needn't handle non-finite values.
Results may differ from the reference program's by a relative error of at most 0.0061.
Values may be sent and summed in bfloat16 or wider, within the bound.
A program may use at most 128 MiB of HBM per device.

```python
import math
import jax
import jax.numpy as jnp
import numpy as np
from jax import lax

D = 2048
CH = 1024
FFE = 1024
CONV_K = 31
TOP = 2
TOK_DEV = 224
TOKENS = 3584
EXPERTS = 16
CAP = 56
N_SP = 16
N_TP = 2


def draw_conv_result(key, part):
    first_key = jax.random.fold_in(jax.random.fold_in(key, 17), 0)
    channel = jnp.arange(CH, dtype=jnp.float32) / CH
    scale = (10.0 ** channel)[None, :]
    values = jnp.clip(jax.random.normal(first_key, (TOKENS, CH), jnp.float32), -6.0, 6.0) * scale
    return values.astype(jnp.bfloat16)


def with_spikes(entries, stream_key, source, target, blocks, factor):
    owner, partner = [(jnp.arange(entries.shape[dim]) // (entries.shape[dim] // blocks)).reshape([-1 if axis == dim else 1 for axis in range(entries.ndim)]) for dim in (source, target)]
    chosen = jax.random.permutation(stream_key, blocks)[partner]
    strong = (owner == chosen) | (owner == (partner + blocks // 2) % blocks)
    return jnp.where(strong, factor * entries, entries)


def steps_of(stream_key, extent, cuts, smallest, high):
    level = 1.0
    for axis_at, shards_of in cuts:
        heights = jax.random.uniform(jax.random.fold_in(jax.random.fold_in(stream_key, 6), axis_at), (shards_of,), jnp.float32, smallest / len(cuts), high / len(cuts))
        level = level * jnp.repeat(jnp.exp(heights), extent[axis_at] // shards_of).reshape((-1,) + (1,) * (len(extent) - 1 - axis_at))
    return level


def deal_out(key, own, number, rows, number_of, top, bound, skew):
    order = jax.random.permutation(key, number_of)
    heavy_load, common = load_shares(number_of, rows * top, bound, skew, True), load_shares(number_of, rows * top, bound, skew, False)
    places = jnp.arange(number_of)

    def named(tallies, offset_by):
        used = int((tallies > 0).sum())
        fixed = max(1, used // 4)
        moved = fixed + (places - fixed + offset_by * (used - fixed)) % max(1, number_of - fixed)
        return jnp.zeros((number_of,), jnp.int32).at[order[jnp.where(places < fixed, places, moved)]].set(jnp.asarray(tallies, jnp.int32))

    tallies = jnp.where(number % 4 == 0, named(heavy_load, number // 4), named(common, number - number // 4 - 1))
    mixed = jax.random.permutation(jax.random.fold_in(own, 3), number_of)
    donor, taker = mixed[0:number_of // 2 * 2:2], mixed[1:number_of // 2 * 2:2]
    margin = jnp.minimum(tallies[donor] - 1, bound - tallies[taker]) // 2
    margin = jnp.where((donor == order[0]) | (taker == order[0]) | (tallies[taker] == 0), 0, jnp.maximum(margin, 0))
    moved = jax.random.randint(jax.random.fold_in(own, 4), (number_of // 2,), 0, 1 << 20) % (margin + 1)
    tallies = tallies.at[donor].add(-moved).at[taker].add(moved)
    members = jnp.searchsorted(jnp.cumsum(tallies), jnp.arange(rows * top), side="right").astype(jnp.int32)
    grid = members.reshape(top, rows).T
    grid = grid[jax.random.permutation(jax.random.fold_in(own, 1), rows)]
    offset_by = jax.random.randint(jax.random.fold_in(own, 2), (rows, 1), 0, top)
    return jnp.take_along_axis(grid, (jnp.arange(top)[None, :] + offset_by) % top, axis=1)


def load_shares(number_of, total, most, slope, full):
    loads = [(1 << 20) // math.isqrt(rank ** slope) + 1 for rank in range(1, number_of + 1)]
    largest = most if full else min(most, max(-(-total // number_of), total * loads[0] // sum(loads)))
    least = 1 if total - largest >= number_of - 1 else 0
    holding, rest = [largest] + [least] * (number_of - 1), total - largest - least * (number_of - 1)
    while rest > 0:
        movable = [i for i in range(1, number_of) if holding[i] < largest] or [i for i in range(1, number_of) if holding[i] < most]
        whole, left = sum([loads[i] for i in movable]), rest
        for i in movable:
            extra = min(most - holding[i], max(1, left * loads[i] // whole), rest)
            holding[i] = holding[i] + extra
            rest = rest - extra
    return np.array(holding)


def centred(key, dims, deviation, limit, pieces=(), kind=jnp.bfloat16):
    drawn = jax.random.normal(key, dims, jnp.float32) * deviation
    if len(pieces) > 0:
        drawn = steps_of(key, dims, pieces, -0.22, 0.18) * drawn
    return jnp.clip(drawn, min=-limit, max=limit).astype(kind)


def gaussian_with(stream_key, extent, width, bound, pieces, heavy, kind=jnp.bfloat16):
    entries = width * jax.random.normal(stream_key, extent, jnp.float32)
    if pieces:
        entries = entries * steps_of(stream_key, extent, pieces, -0.22, 0.18)
    return jnp.clip(with_spikes(entries, jax.random.fold_in(stream_key, 3), *heavy), -bound, bound).astype(kind)


def setup_inputs(seed: int = 0) -> dict:
    seeds = jax.random.split(jax.random.key(seed), 14)
    out_grad = gaussian_with(seeds[0], (TOKENS, D), 1.0, 6.0, ((0, 16),), (0, 1, 16, 2.0))
    moe_input = centred(seeds[1], (TOKENS, D), 1.0, 6.0, ((0, 16),))
    routes_keys = jax.random.split(jax.random.fold_in(seeds[2], 1), TOKENS // TOK_DEV)
    routes_turns = jax.random.permutation(jax.random.fold_in(seeds[2], 3), TOKENS // TOK_DEV)
    routes = jax.vmap(lambda own, number: deal_out(jax.random.fold_in(seeds[2], 2), own, number, TOK_DEV, EXPERTS, TOP, CAP, 1))(routes_keys, routes_turns).reshape((TOKENS, TOP))
    route_weights = jnp.clip(0.2 + 0.8 * jax.random.uniform(seeds[3], (TOKENS, TOP), jnp.float32) ** steps_of(seeds[3], (TOKENS, TOP), ((0, 16),), -0.2, 0.2), 0.2, 1.0)
    conv_result = draw_conv_result(jax.random.fold_in(seeds[13], 71), 0)
    glu_value = centred(seeds[5], (TOKENS, CH), 1.0, 6.0, ((0, 16), (1, 2)))
    glu_gate = centred(seeds[6], (TOKENS, CH), 1.0, 6.0, ((0, 16), (1, 2)))
    conv_taps = centred(seeds[7], (CONV_K, CH), CONV_K ** -0.5, 1.0, ((1, 2),))
    norm_gain = jnp.clip(1.0 + 0.18 * jax.random.normal(seeds[8], (CH,), jnp.float32), 0.1, 1.9)
    proj_weight = centred(seeds[9], (D, CH), CH ** -0.5, 0.1875, ((1, 2),))
    expert_gate = centred(seeds[10], (EXPERTS, D, FFE), D ** -0.5, 0.125, ((0, 16), (2, 2)))
    expert_up = centred(seeds[11], (EXPERTS, D, FFE), D ** -0.5, 0.125, ((0, 16), (2, 2)))
    expert_down = centred(seeds[12], (EXPERTS, FFE, D), FFE ** -0.5, 0.1875, ((0, 16), (1, 2)))
    return dict(out_grad=out_grad, moe_input=moe_input, routes=routes, route_weights=route_weights, conv_result=conv_result, glu_value=glu_value, glu_gate=glu_gate, conv_taps=conv_taps, norm_gain=norm_gain, proj_weight=proj_weight, expert_gate=expert_gate, expert_up=expert_up, expert_down=expert_down)


norm_eps = 1e-05

def contract_rows(left, right):
    return lax.dot_general(left, right, (((0,), (0,)), ((), ())), preferred_element_type=jnp.float32)

def reference(out_grad, moe_input, routes, route_weights, conv_result, glu_value, glu_gate, conv_taps, norm_gain, proj_weight, expert_gate, expert_up, expert_down):
    slots = N_SP * CAP
    assigned = TOKENS * TOP
    flat = routes.reshape(N_SP, TOK_DEV * TOP).astype(jnp.int32)
    onehot = (flat[:, :, None] == jnp.arange(EXPERTS, dtype=jnp.int32)[None, None, :]).astype(jnp.int32)
    earlier = jnp.cumsum(onehot, axis=1) - onehot
    slot_index = lax.optimization_barrier(jnp.sum(earlier * onehot, axis=2))
    position = (jnp.arange(N_SP, dtype=jnp.int32)[:, None] * CAP + slot_index).reshape(-1).astype(jnp.int32)
    expert_flat = flat.reshape(-1)
    table = jnp.full((EXPERTS, slots), assigned, jnp.int32).at[expert_flat, position].set(jnp.arange(assigned, dtype=jnp.int32))
    grad_padded = jnp.concatenate([out_grad, jnp.zeros((1, D), jnp.bfloat16)], axis=0)
    input_padded = jnp.concatenate([moe_input, jnp.zeros((1, D), jnp.bfloat16)], axis=0)
    weight_padded = jnp.concatenate([route_weights.reshape(-1), jnp.zeros((1,), jnp.float32)])
    row_scale = float(slots) ** (-0.5)
    piece = FFE // N_TP

    def per_expert(args):
        index, weight_g, weight_u, weight_d = args
        token = jnp.where(index < assigned, index // TOP, TOKENS).astype(jnp.int32)
        inputs = input_padded[token]
        grads = (grad_padded[token].astype(jnp.float32) * weight_padded[index][:, None]).astype(jnp.bfloat16)
        gate_pre = jnp.dot(inputs, weight_g, preferred_element_type=jnp.float32)
        up_pre = jnp.dot(inputs, weight_u, preferred_element_type=jnp.float32)
        sigma = jax.nn.sigmoid(gate_pre)
        silu_gate = gate_pre * sigma
        hidden = (silu_gate * up_pre).astype(jnp.bfloat16)
        down_g = contract_rows(hidden, grads) * row_scale
        hidden_grad = lax.dot_general(grads, weight_d, (((1,), (1,)), ((), ())), preferred_element_type=jnp.float32)
        gate_back = (hidden_grad * up_pre * sigma * (1.0 + gate_pre * (1.0 - sigma))).astype(jnp.bfloat16)
        up_back = (hidden_grad * silu_gate).astype(jnp.bfloat16)
        gate_g = contract_rows(inputs, gate_back) * row_scale
        up_g = contract_rows(inputs, up_back) * row_scale
        back_gate = jnp.einsum('rpf,dpf->prd', gate_back.reshape(slots, N_TP, piece).astype(jnp.float32), weight_g.reshape(D, N_TP, piece).astype(jnp.float32))
        back_up = jnp.einsum('rpf,dpf->prd', up_back.reshape(slots, N_TP, piece).astype(jnp.float32), weight_u.reshape(D, N_TP, piece).astype(jnp.float32))
        partial_value = lax.optimization_barrier((back_gate + back_up).astype(jnp.bfloat16)).astype(jnp.float32)
        rows_back = lax.optimization_barrier(jnp.sum(partial_value, axis=0)).astype(jnp.bfloat16)
        return (gate_g, up_g, down_g, rows_back)
    gate_grad, up_grad, down_grad, returned = lax.map(per_expert, (table, expert_gate, expert_up, expert_down))
    contrib = returned.reshape(EXPERTS * slots, D)[(expert_flat * slots + position).astype(jnp.int32)]
    total = out_grad.astype(jnp.float32) + lax.optimization_barrier(jnp.sum(contrib.reshape(TOKENS, TOP, D).astype(jnp.float32), axis=1))
    input_grad = total.astype(jnp.bfloat16)
    values = conv_result.astype(jnp.float32)
    center = lax.optimization_barrier(jnp.mean(values, axis=1, keepdims=True))
    spread = lax.optimization_barrier(jnp.mean(values * values, axis=1, keepdims=True)) - center * center
    inv_std = lax.rsqrt(spread + norm_eps)
    normed = (values - center) * inv_std
    scaled = normed * norm_gain[None, :]
    sig_norm = jax.nn.sigmoid(scaled)
    activ = (scaled * sig_norm).astype(jnp.bfloat16)
    proj_grad = contract_rows(input_grad, activ) * float(TOKENS) ** (-0.5)
    act_grad = jnp.dot(input_grad, proj_weight, preferred_element_type=jnp.float32)
    norm_grad = act_grad * sig_norm * (1.0 + scaled * (1.0 - sig_norm)) * norm_gain[None, :]
    first = lax.optimization_barrier(jnp.mean(norm_grad, axis=1, keepdims=True))
    second = lax.optimization_barrier(jnp.mean(norm_grad * normed, axis=1, keepdims=True))
    conv_grad = inv_std * (norm_grad - first - normed * second)
    extended = jnp.concatenate([conv_grad, jnp.zeros((CONV_K - 1, CH), jnp.float32)], axis=0)
    taps_float = conv_taps.astype(jnp.float32)
    mixed_grad = jnp.zeros((TOKENS, CH), jnp.float32)
    for lag in range(CONV_K):
        mixed_grad = mixed_grad + taps_float[CONV_K - 1 - lag][None, :] * extended[lag:lag + TOKENS]
    sig_gate = jax.nn.sigmoid(glu_gate.astype(jnp.float32))
    value_grad = (mixed_grad * sig_gate).astype(jnp.bfloat16)
    gate_side_grad = (mixed_grad * glu_value.astype(jnp.float32) * sig_gate * (1.0 - sig_gate)).astype(jnp.bfloat16)
    return (input_grad, proj_grad, gate_grad, up_grad, down_grad, value_grad, gate_side_grad)
```

```python
import functools

import jax
import jax.numpy as jnp
from jax import lax
from jax.experimental import pallas as pl
from jax.experimental.pallas import tpu as pltpu
from jax.sharding import PartitionSpec as P

norm_eps = 1e-05
MESH = pl.DeviceIdType.MESH
LANES = 128
STRIP = 32


def contract_rows(left, right):
    return lax.dot_general(
        left, right, (((0,), (0,)), ((), ())), preferred_element_type=jnp.float32
    )


def contract_cols(left, right):
    return lax.dot_general(
        left, right, (((1,), (1,)), ((), ())), preferred_element_type=jnp.float32
    )


def remote(src, dst, send, recv, where):
    return pltpu.make_async_remote_copy(
        src_ref=src,
        dst_ref=dst,
        send_sem=send,
        recv_sem=recv,
        device_id=where,
        device_id_type=MESH,
    )


def signal(sem, where):
    pl.semaphore_signal(sem, inc=1, device_id=where, device_id_type=MESH)


def two_lanes(first, second):
    lane = lax.broadcasted_iota(jnp.int32, (first.shape[0], LANES), 1)
    return jnp.where(lane == 0, first, jnp.where(lane == 1, second, 0.0))


def dispatch_body(
    n, group, channels, xin, xgr, conv, gain, outs_in, outs_gr, act_out, stat_out,
    sums_mine, sums_other, act_src, own_sem, send_sem, recv_sem, fwd_send, fwd_recv,
    act_sem, act_send, act_recv, act_fsend, act_frecv, sum_sem,
):
    xs, outs = (xin, xgr), (outs_in, outs_gr)
    me, half = lax.axis_index("sp"), lax.axis_index("tp")
    other = 1 - half
    base, mine = me // group * group, lax.rem(me, group)
    rows, width = conv.shape

    def place(a, source, side):
        cols = xs[a].shape[2]
        return outs[a].at[source, :, pl.ds(pl.multiple_of(side * cols, cols), cols)]

    def act_place(source, side):
        return act_out.at[source, :, pl.ds(pl.multiple_of(side * width, width), width)]

    def outgoing(a, step):
        peer = lax.rem(me + step, n)
        return remote(
            xs[a].at[peer], place(a, me, half), send_sem.at[a, step], recv_sem.at[a, step],
            (peer, half),
        )

    def incoming(a, step):
        source = lax.rem(me + n - step, n)
        return remote(
            xs[a].at[source], place(a, source, half), send_sem.at[a, step], recv_sem.at[a, step],
            (source, half),
        )

    def relayed(a, step):
        source = lax.rem(me + n - step, n)
        return remote(
            place(a, source, half), place(a, source, half), fwd_send.at[a, step],
            fwd_recv.at[a, step], (me, other),
        )

    def first_relay(a):
        return remote(
            xs[a].at[me], place(a, me, half), fwd_send.at[a, 0], fwd_recv.at[a, 0], (me, other)
        )

    def from_other(a, step):
        source = lax.rem(me + n - step, n)
        return remote(
            xs[a].at[source], place(a, source, other), fwd_send.at[a, step],
            fwd_recv.at[a, step], (me, other),
        )

    def act_outgoing(step):
        peer = base + lax.rem(mine + step, group)
        return remote(
            act_src, act_place(mine, half), act_send.at[step], act_recv.at[step], (peer, half)
        )

    def act_incoming(step):
        source = lax.rem(mine + group - step, group)
        return remote(
            act_src, act_place(source, half), act_send.at[step], act_recv.at[step],
            (base + source, half),
        )

    def act_relayed(step):
        source = lax.rem(mine + group - step, group)
        return remote(
            act_place(source, half), act_place(source, half), act_fsend.at[step],
            act_frecv.at[step], (me, other),
        )

    def act_first():
        return remote(
            act_src, act_place(mine, half), act_fsend.at[0], act_frecv.at[0], (me, other)
        )

    def act_from_other(step):
        source = lax.rem(mine + group - step, group)
        return remote(
            act_src, act_place(source, other), act_fsend.at[step], act_frecv.at[step],
            (me, other),
        )

    def loop(first, last, body):
        def step(i, carry):
            body(i)
            return carry

        lax.fori_loop(first, last, step, 0)

    barrier = pltpu.get_barrier_semaphore()
    loop(1, n, lambda step: signal(barrier, (lax.rem(me + step, n), half)))
    signal(barrier, (me, other))
    pl.semaphore_wait(barrier, n)

    for a in range(2):
        loop(1, n, lambda step, a=a: outgoing(a, step).start())
    own = []
    for a in range(2):
        own.append(pltpu.make_async_copy(xs[a].at[me], place(a, me, half), own_sem.at[a]))
        own[-1].start()
        first_relay(a).start()

    def strip(i):
        return pl.ds(pl.multiple_of(i * STRIP, STRIP), STRIP)

    def statistics(i):
        values = conv[strip(i), :].astype(jnp.float32)
        sums_mine[strip(i), :] = two_lanes(
            jnp.sum(values, axis=1, keepdims=True),
            jnp.sum(values * values, axis=1, keepdims=True),
        )

    loop(0, rows // STRIP, statistics)
    both = remote(sums_mine, sums_other, sum_sem.at[0], sum_sem.at[1], (me, other))
    both.start()
    both.wait()

    def activate(i):
        total = sums_mine[strip(i), :] + sums_other[strip(i), :]
        center = total[:, 0:1] / channels
        spread = total[:, 1:2] / channels - center * center
        inv_std = lax.rsqrt(spread + norm_eps)
        stat_out[strip(i), :] = two_lanes(center, inv_std)
        scaled = (conv[strip(i), :].astype(jnp.float32) - center) * inv_std * gain[...]
        act_src[strip(i), :] = (scaled * jax.nn.sigmoid(scaled)).astype(jnp.bfloat16)

    loop(0, rows // STRIP, activate)
    own.append(pltpu.make_async_copy(act_src, act_place(mine, half), act_sem))
    own[-1].start()
    loop(1, group, lambda step: act_outgoing(step).start())
    act_first().start()

    def arrive(a, step):
        incoming(a, step).wait_recv()
        relayed(a, step).start()

    loop(1, n, lambda step: arrive(0, step))

    def act_arrive(step):
        act_incoming(step).wait_recv()
        act_relayed(step).start()

    loop(1, group, act_arrive)
    loop(1, n, lambda step: arrive(1, step))

    for a in range(2):

        def finish(step, a=a):
            outgoing(a, step).wait_send()
            relayed(a, step).wait_send()
            from_other(a, step).wait_recv()

        loop(1, n, finish)
        first_relay(a).wait_send()
        from_other(a, 0).wait_recv()

    def act_finish(step):
        act_outgoing(step).wait_send()
        act_relayed(step).wait_send()
        act_from_other(step).wait_recv()

    loop(1, group, act_finish)
    act_first().wait_send()
    act_from_other(0).wait_recv()
    for copy in own:
        copy.wait()


def dispatch(send_input, send_grad, conv_result, gain, group, channels, collective_id):
    n = send_input.shape[0]
    rows, width = conv_result.shape
    wide = jax.ShapeDtypeStruct(
        (n, send_input.shape[1], 2 * send_input.shape[2]), send_input.dtype
    )
    dma = pltpu.SemaphoreType.DMA
    vmem = pl.BlockSpec(memory_space=pltpu.VMEM)
    anywhere = pl.BlockSpec(memory_space=pl.ANY)
    return pl.pallas_call(
        functools.partial(dispatch_body, n, group, channels),
        out_shape=(
            wide,
            wide,
            jax.ShapeDtypeStruct((group, rows, 2 * width), jnp.bfloat16),
            jax.ShapeDtypeStruct((rows, LANES), jnp.float32),
        ),
        in_specs=[vmem] * 4,
        out_specs=(anywhere, anywhere, anywhere, vmem),
        scratch_shapes=[
            pltpu.VMEM((rows, LANES), jnp.float32),
            pltpu.VMEM((rows, LANES), jnp.float32),
            pltpu.VMEM((rows, width), jnp.bfloat16),
            dma((2,)),
            dma((2, n)),
            dma((2, n)),
            dma((2, n)),
            dma((2, n)),
            dma,
            dma((group,)),
            dma((group,)),
            dma((group,)),
            dma((group,)),
            dma((2,)),
        ],
        compiler_params=pltpu.CompilerParams(collective_id=collective_id, has_side_effects=True),
    )(send_input, send_grad, conv_result, gain)


def giveback_body(n, x, out, own_sem, send_sem, recv_sem):
    me, half = lax.axis_index("sp"), lax.axis_index("tp")

    def outgoing(step):
        peer = lax.rem(me + step, n)
        return remote(
            x.at[peer], out.at[me], send_sem.at[step], recv_sem.at[step], (peer, half)
        )

    def incoming(step):
        source = lax.rem(me + n - step, n)
        return remote(
            x.at[source], out.at[source], send_sem.at[step], recv_sem.at[step], (source, half)
        )

    barrier = pltpu.get_barrier_semaphore()

    def loop(body):
        def step(i, carry):
            body(i)
            return carry

        lax.fori_loop(1, n, step, 0)

    loop(lambda step: signal(barrier, (lax.rem(me + step, n), half)))
    pl.semaphore_wait(barrier, n - 1)
    loop(lambda step: outgoing(step).start())
    own = pltpu.make_async_copy(x.at[me], out.at[me], own_sem)
    own.start()

    def finish(step):
        incoming(step).wait_recv()
        outgoing(step).wait_send()

    loop(finish)
    own.wait()


def giveback(x, collective_id):
    n = x.shape[0]
    dma = pltpu.SemaphoreType.DMA
    return pl.pallas_call(
        functools.partial(giveback_body, n),
        out_shape=jax.ShapeDtypeStruct(x.shape, x.dtype),
        in_specs=[pl.BlockSpec(memory_space=pltpu.VMEM)],
        out_specs=pl.BlockSpec(memory_space=pltpu.VMEM),
        scratch_shapes=[dma, dma((n,)), dma((n,))],
        compiler_params=pltpu.CompilerParams(collective_id=collective_id, has_side_effects=True),
    )(x)


def tail_body(
    n, group, reach, token_scale, channels,
    share, feats, act, proj_w, conv, stat, gain, taps, value, gate,
    igrad, pgrad, vgrad, ggrad,
    feat_buf, sums_mine, sums_other, ext, halo_src, halo_buf, piece, rs_buf,
    local_sem, pair_sem, feat_send, feat_recv, piece_send, piece_recv, halo_sem,
):
    me, half = lax.axis_index("sp"), lax.axis_index("tp")
    other = 1 - half
    mine, my_group = lax.rem(me, group), me // group
    base = my_group * group
    groups = n // group
    per_half = groups // 2
    rows, share_width = share.shape
    width = conv.shape[1]
    piece_rows = feats.shape[2] // per_half
    rim = halo_src.shape[0]
    last = n - 1

    def loop(first, end, body):
        def step(i, carry):
            body(i)
            return carry

        lax.fori_loop(first, end, step, 0)

    def strip(i):
        return pl.ds(pl.multiple_of(i * STRIP, STRIP), STRIP)

    barrier = pltpu.get_barrier_semaphore()
    signal(barrier, (me, other))
    for step in range(1, group):
        signal(barrier, (base + lax.rem(mine + step, group), half))
    for step in range(1, groups):
        for side in range(2):
            signal(barrier, (lax.rem(my_group + step, groups) * group + mine, side))

    @pl.when(me > 0)
    def _():
        signal(barrier, (me - 1, half))

    @pl.when(me < last)
    def _():
        signal(barrier, (me + 1, half))

    ends = jnp.where(me > 0, 1, 0) + jnp.where(me < last, 1, 0)
    pl.semaphore_wait(barrier, 1 + (group - 1) + 2 * (groups - 1) + ends)

    def side_cols(side):
        return pl.ds(pl.multiple_of(side * share_width, share_width), share_width)

    to_pair = remote(
        share, igrad.at[:, side_cols(half)], pair_sem.at[0], pair_sem.at[1], (me, other)
    )
    to_pair.start()
    keep = pltpu.make_async_copy(share, igrad.at[:, side_cols(half)], local_sem.at[0])
    keep.start()

    def feat_out(step):
        peer = lax.rem(mine + step, group)
        return remote(
            feats.at[peer], feat_buf.at[mine], feat_send.at[step], feat_recv.at[step],
            (base + peer, half),
        )

    def feat_in(step):
        source = lax.rem(mine + group - step, group)
        return remote(
            feats.at[source], feat_buf.at[source], feat_send.at[step], feat_recv.at[step],
            (base + source, half),
        )

    for step in range(1, group):
        feat_out(step).start()
    keep_feat = pltpu.make_async_copy(feats.at[mine], feat_buf.at[mine], local_sem.at[1])
    keep_feat.start()

    keep.wait()
    to_pair.wait()
    ext[0:rows, :] = jnp.dot(igrad[...], proj_w[...], preferred_element_type=jnp.float32)

    def normed_of(i):
        center, inv_std = stat[strip(i), 0:1], stat[strip(i), 1:2]
        return (conv[strip(i), :].astype(jnp.float32) - center) * inv_std, inv_std

    def norm_back(i):
        normed, _ = normed_of(i)
        scaled = normed * gain[...]
        sig = jax.nn.sigmoid(scaled)
        back = ext[strip(i), :] * sig * (1.0 + scaled * (1.0 - sig)) * gain[...]
        ext[strip(i), :] = back
        sums_mine[strip(i), :] = two_lanes(
            jnp.sum(back, axis=1, keepdims=True), jnp.sum(back * normed, axis=1, keepdims=True)
        )

    loop(0, rows // STRIP, norm_back)
    sums = remote(sums_mine, sums_other, pair_sem.at[2], pair_sem.at[3], (me, other))
    sums.start()

    keep_feat.wait()
    for step in range(1, group):
        feat_in(step).wait_recv()
    received = feat_buf[...].reshape(group * rows, feats.shape[2])

    def piece_out(q, side, where):
        return remote(
            piece.at[q, side], rs_buf.at[my_group], piece_send.at[q, side],
            piece_recv.at[my_group], (where * group + mine, side),
        )

    def piece_keep(q, side):
        return pltpu.make_async_copy(piece.at[q, side], rs_buf.at[my_group], local_sem.at[2])

    def each_piece(sides, at_home, away):
        for side in sides:
            for q in range(per_half):
                where = half * per_half + q
                home = jnp.logical_and(where == my_group, half == side)

                @pl.when(home)
                def _(q=q, side=side):
                    at_home(q, side)

                @pl.when(jnp.logical_not(home))
                def _(q=q, side=side, where=where):
                    away(q, side, where)

    for side in range(2):
        partial = contract_rows(
            received, act[:, side * width : (side + 1) * width]
        ).astype(jnp.bfloat16)
        for q in range(per_half):
            piece[q, side] = partial[q * piece_rows : (q + 1) * piece_rows]
    each_piece(
        range(2),
        lambda q, side: piece_keep(q, side).start(),
        lambda q, side, where: piece_out(q, side, where).start(),
    )

    sums.wait()

    def conv_back(i):
        normed, inv_std = normed_of(i)
        total = (sums_mine[strip(i), :] + sums_other[strip(i), :]) / channels
        ext[strip(i), :] = inv_std * (
            ext[strip(i), :] - total[:, 0:1] - normed * total[:, 1:2]
        )

    loop(0, rows // STRIP, conv_back)
    halo_src[...] = ext[0:rim, :].astype(jnp.bfloat16)

    def halo_copy(where):
        return remote(halo_src, halo_buf, halo_sem.at[0], halo_sem.at[1], (where, half))

    @pl.when(me > 0)
    def _():
        halo_copy(me - 1).start()

    @pl.when(me < last)
    def _():
        halo_copy(me + 1).wait_recv()
        ext[rows : rows + rim, :] = halo_buf[...].astype(jnp.float32)

    @pl.when(me == last)
    def _():
        ext[rows : rows + rim, :] = jnp.zeros((rim, width), jnp.float32)

    def convolve(c):
        cols = pl.ds(pl.multiple_of(c * LANES, LANES), LANES)
        mixed = jnp.zeros((rows, LANES), jnp.float32)
        for lag in range(reach):
            tap = taps[reach - 1 - lag : reach - lag, cols]
            mixed = mixed + tap * ext[lag : lag + rows, cols]
        sig = jax.nn.sigmoid(gate[:, cols].astype(jnp.float32))
        vgrad[:, cols] = (mixed * sig).astype(jnp.bfloat16)
        ggrad[:, cols] = (
            mixed * value[:, cols].astype(jnp.float32) * sig * (1.0 - sig)
        ).astype(jnp.bfloat16)

    loop(0, width // LANES, convolve)

    def piece_in(source):
        return remote(
            piece.at[0, 0], rs_buf.at[source], piece_send.at[0, 0], piece_recv.at[source],
            (source * group + mine, half),
        )

    my_half = my_group // per_half
    for source in range(groups):

        @pl.when(jnp.logical_not(jnp.logical_and(source == my_group, half == my_half)))
        def _(source=source):
            piece_in(source).wait_recv()

    each_piece(
        range(2),
        lambda q, side: piece_keep(q, side).wait(),
        lambda q, side, where: piece_out(q, side, where).wait_send(),
    )
    total = rs_buf[0].astype(jnp.float32)
    for source in range(1, groups):
        total = total + rs_buf[source].astype(jnp.float32)
    pgrad[...] = total * token_scale

    for step in range(1, group):
        feat_out(step).wait_send()

    @pl.when(me > 0)
    def _():
        halo_copy(me - 1).wait_send()


def tail(
    share, feats, act, proj_w, conv, stat, gain, taps, value, gate, n, token_scale, channels,
    collective_id,
):
    group, rows, wide = feats.shape
    width = conv.shape[1]
    groups = n // group
    per_half = groups // 2
    piece_rows = wide // per_half
    reach = taps.shape[0]
    rim = -(-(reach - 1) // 16) * 16
    dma = pltpu.SemaphoreType.DMA
    vmem = pl.BlockSpec(memory_space=pltpu.VMEM)
    return pl.pallas_call(
        functools.partial(tail_body, n, group, reach, token_scale, channels),
        out_shape=(
            jax.ShapeDtypeStruct((rows, 2 * share.shape[1]), jnp.bfloat16),
            jax.ShapeDtypeStruct((piece_rows, width), jnp.float32),
            jax.ShapeDtypeStruct((rows, width), jnp.bfloat16),
            jax.ShapeDtypeStruct((rows, width), jnp.bfloat16),
        ),
        in_specs=[vmem] * 10,
        out_specs=(vmem,) * 4,
        scratch_shapes=[
            pltpu.VMEM((group, rows, wide), jnp.bfloat16),
            pltpu.VMEM((rows, LANES), jnp.float32),
            pltpu.VMEM((rows, LANES), jnp.float32),
            pltpu.VMEM((rows + rim, width), jnp.float32),
            pltpu.VMEM((rim, width), jnp.bfloat16),
            pltpu.VMEM((rim, width), jnp.bfloat16),
            pltpu.VMEM((per_half, 2, piece_rows, width), jnp.bfloat16),
            pltpu.VMEM((groups, piece_rows, width), jnp.bfloat16),
            dma((3,)),
            dma((4,)),
            dma((group,)),
            dma((group,)),
            dma((per_half, 2)),
            dma((groups,)),
            dma((2,)),
        ],
        compiler_params=pltpu.CompilerParams(collective_id=collective_id, has_side_effects=True),
    )(share, feats, act, proj_w, conv, stat, gain, taps, value, gate)


def per_device(
    out_grad,
    moe_input,
    routes,
    route_weights,
    conv_result,
    glu_value,
    glu_gate,
    conv_taps,
    norm_gain,
    proj_weight,
    expert_gate,
    expert_up,
    expert_down,
):
    n_sp = lax.axis_size("sp")
    n_tp = lax.axis_size("tp")
    half = lax.axis_index("tp")
    tok_rows, width = out_grad.shape
    top_count = routes.shape[1]
    bound = 2 * top_count * tok_rows // n_sp
    capacity = -(-bound // 8) * 8
    slots = n_sp * capacity
    share = width // n_tp
    channels = conv_result.shape[1] * n_tp
    group = n_sp // 4
    gain = norm_gain[None, :]
    experts = jnp.arange(n_sp, dtype=jnp.int32)[None, :]
    named = [(routes[:, k : k + 1] == experts) for k in range(top_count)]
    per_token = sum(hit.astype(jnp.bfloat16) for hit in named)
    order = jnp.arange(tok_rows, dtype=jnp.int32)
    before = (order[None, :] < order[:, None]).astype(jnp.bfloat16)
    earlier = jnp.dot(before, per_token, preferred_element_type=jnp.float32).astype(jnp.int32)
    rows = jnp.arange(slots, dtype=jnp.int32)
    chosen = []
    for k in range(top_count):
        slot = jnp.sum(jnp.where(named[k], earlier, 0), axis=1)
        target = routes[:, k] * capacity + slot
        chosen.append(rows[:, None] == target[None, :])
    pick = functools.reduce(jnp.logical_or, chosen).astype(jnp.bfloat16)
    row_weight = sum(
        jnp.sum(jnp.where(chosen[k], route_weights[:, k][None, :], 0.0), axis=1)
        for k in range(top_count)
    )
    input_half = lax.dynamic_slice_in_dim(moe_input, half * share, share, 1)
    grad_half = lax.dynamic_slice_in_dim(out_grad, half * share, share, 1)
    send_input = jnp.dot(pick, input_half, preferred_element_type=jnp.float32).astype(jnp.bfloat16)
    send_grad = (
        jnp.dot(pick, grad_half, preferred_element_type=jnp.float32) * row_weight[:, None]
    ).astype(jnp.bfloat16)
    row_scale = float(n_sp * bound) ** (-0.5)
    blocks = (n_sp, capacity, share)
    inputs, grads, all_act, stat = dispatch(
        send_input.reshape(blocks), send_grad.reshape(blocks), conv_result, gain, group,
        channels, 1,
    )
    inputs, grads = inputs.reshape(slots, width), grads.reshape(slots, width)

    gate_pre = jnp.dot(inputs, expert_gate[0], preferred_element_type=jnp.float32)
    up_pre = jnp.dot(inputs, expert_up[0], preferred_element_type=jnp.float32)
    sigma = jax.nn.sigmoid(gate_pre)
    silu_gate = gate_pre * sigma
    hidden = (silu_gate * up_pre).astype(jnp.bfloat16)
    down_g = contract_rows(hidden, grads) * row_scale
    hidden_grad = contract_cols(grads, expert_down[0])
    gate_back = (hidden_grad * up_pre * sigma * (1.0 + gate_pre * (1.0 - sigma))).astype(
        jnp.bfloat16
    )
    up_back = (hidden_grad * silu_gate).astype(jnp.bfloat16)
    gate_g = contract_rows(inputs, gate_back) * row_scale
    up_g = contract_rows(inputs, up_back) * row_scale

    def partial_of(side):
        weight_g = lax.dynamic_slice_in_dim(expert_gate[0], side * share, share, 0)
        weight_u = lax.dynamic_slice_in_dim(expert_up[0], side * share, share, 0)
        return (contract_cols(gate_back, weight_g) + contract_cols(up_back, weight_u)).astype(
            jnp.bfloat16
        )

    arrived = lax.ppermute(
        partial_of(1 - half), "tp", [(i, n_tp - 1 - i) for i in range(n_tp)]
    )
    summed = (partial_of(half).astype(jnp.float32) + arrived.astype(jnp.float32)).astype(
        jnp.bfloat16
    )
    returned = giveback(summed.reshape(blocks), 2).reshape(slots, share)
    grad_share = (grad_half.astype(jnp.float32) + contract_rows(pick, returned)).astype(
        jnp.bfloat16
    )
    groups = n_sp // group
    feature = width // n_sp
    per_half = groups // n_tp
    feats = (
        grad_share.reshape(tok_rows, per_half, group, feature)
        .transpose(2, 0, 1, 3)
        .reshape(group, tok_rows, per_half * feature)
    )
    input_grad, proj_grad, value_grad, gate_side_grad = tail(
        grad_share, feats, all_act.reshape(group * tok_rows, channels), proj_weight,
        conv_result, stat, gain, conv_taps.astype(jnp.float32), glu_value, glu_gate, n_sp,
        float(tok_rows * n_sp) ** (-0.5), channels, 3,
    )
    return (
        input_grad,
        proj_grad,
        gate_g[None],
        up_g[None],
        down_g[None],
        value_grad,
        gate_side_grad,
    )


def solution(mesh):
    in_specs = (
        P("sp", None),
        P("sp", None),
        P("sp", None),
        P("sp", None),
        P("sp", "tp"),
        P("sp", "tp"),
        P("sp", "tp"),
        P(None, "tp"),
        P("tp"),
        P(None, "tp"),
        P("sp", None, "tp"),
        P("sp", None, "tp"),
        P("sp", "tp", None),
    )
    out_specs = (
        P("sp", None),
        P("sp", "tp"),
        P("sp", None, "tp"),
        P("sp", None, "tp"),
        P("sp", "tp", None),
        P("sp", "tp"),
        P("sp", "tp"),
    )
    return jax.shard_map(
        per_device, mesh=mesh, in_specs=in_specs, out_specs=out_specs, check_vma=False
    )
```
